32 devices in a mesh: sp: 4 (over y, core), tp: 8 (over z, x).
Axes of the slice: x: 2, y: 2, z: 4, core: 2. Of those that a mesh axis runs over, the one named last changes fastest.
Arguments:
- queries: bfloat16 [512, 3072], P('sp'), may hold values from -6 to 6
- attn_out: bfloat16 [512, 3072], P('sp'), may hold values from -3 to 3
- log_norm: float32 [512, 12], P('sp'), as said below
- cotangent: bfloat16 [512, 3072], P('sp'), may hold values from -96 to 96
- keys: bfloat16 [1024, 512], P(('sp', 'tp')), may hold values from -6 to 6
- values: bfloat16 [1024, 512], P(('sp', 'tp')), may hold values from -6 to 6
- source: bfloat16 [1024, 3072], P('sp', 'tp'), may hold values from -6 to 6
- w_query: bfloat16 [3072, 3072], P('tp'), may hold values from -0.109375 to 0.109375
- w_key: bfloat16 [3072, 512], P('tp'), may hold values from -0.109375 to 0.109375
- w_value: bfloat16 [3072, 512], P('tp'), may hold values from -0.109375 to 0.109375
Outputs:
- d_target: bfloat16 [512, 3072], P('sp', 'tp')
- d_source: bfloat16 [1024, 3072], P('sp', 'tp')
- d_wvalue: float32 [3072, 512], P('tp')
The draws below stay inside these ranges and needn't reach their ends.
Inputs may be any that keep to these rules, and one draw needn't show every extreme that they name: `log_norm`: the logarithm of the softmax total saved by the forward pass, near log(1024) + 0.5.
All inputs are finite; a program needn't handle non-finite values.
Results may differ from the reference program's by a relative error of at most 0.024.
Values may be sent and summed in bfloat16 or wider, within the bound.
No kernel may reach another device: no remote copies, remote signals or barrier semaphores. Data moves between devices by JAX's collectives and lax.ppermute only.
A program may use at most 64 MiB of HBM per device.

```python
import math
import jax
import jax.numpy as jnp
from jax import lax

HEADS = 12
KV_HEADS = 2
HEAD_DIM = 256
TARGET_ROWS_EACH = 128
D = 3072
KW = 512
TGT = 512
SRC = 1024


def draw_log_norm(key, part):
    center = math.log(SRC) + 0.5
    spread = jax.random.uniform(key, (TGT, HEADS), jnp.float32, -0.5, 0.5)
    return (center + spread).astype(jnp.float32)


def level_of(key, dims, cuts, low, largest):
    def one(dim, blocks):
        heights = jax.random.uniform(jax.random.fold_in(jax.random.fold_in(key, 6), dim), (blocks,), jnp.float32, low / len(cuts), largest / len(cuts))
        return jnp.repeat(jnp.exp(heights), dims[dim] // blocks).reshape((-1,) + (1,) * (len(dims) - dim - 1))

    level = one(*cuts[0])
    for cut in cuts[1:]:
        level = level * one(*cut)
    return level


def scatter_about(own_key, extent, deviation, limit, shards=(), kind=jnp.bfloat16):
    factor_of = level_of(own_key, extent, shards, -0.22, 0.18) if shards else 1.0
    values = jax.random.normal(own_key, extent, jnp.float32) * deviation * factor_of
    return jnp.minimum(jnp.maximum(values, -limit), limit).astype(kind)


def setup_inputs(seed: int = 0) -> dict:
    splits = jax.random.split(jax.random.key(seed), 11)
    return {
        "queries": scatter_about(splits[0], (TGT, D), 1.0, 6.0, ((0, 4),)),
        "attn_out": scatter_about(splits[1], (TGT, D), 0.5, 3.0, ((0, 4),)),
        "log_norm": draw_log_norm(jax.random.fold_in(splits[10], 71), 0),
        "cotangent": scatter_about(splits[3], (TGT, D), 16.0, 96.0, ((0, 4),)),
        "keys": scatter_about(splits[4], (SRC, KW), 1.0, 6.0, ((0, 32),)),
        "values": scatter_about(splits[5], (SRC, KW), 1.0, 6.0, ((0, 32),)),
        "source": scatter_about(splits[6], (SRC, D), 1.0, 6.0, ((0, 4), (1, 8))),
        "w_query": scatter_about(splits[7], (D, D), D ** -0.5, 0.109375, ((0, 8),)),
        "w_key": scatter_about(splits[8], (D, KW), D ** -0.5, 0.109375, ((0, 8),)),
        "w_value": scatter_about(splits[9], (D, KW), D ** -0.5, 0.109375, ((0, 8),)),
    }


def reference(queries, attn_out, log_norm, cotangent, keys, values, source, w_query, w_key, w_value):
    single_precision = jnp.float32
    repeat = HEADS // KV_HEADS
    score_scale = 1.0 / math.sqrt(HEAD_DIM)
    src_rows = keys.shape[0]
    shared_key_heads = keys.astype(single_precision).reshape(src_rows, KV_HEADS, HEAD_DIM)
    shared_value_heads = values.astype(single_precision).reshape(src_rows, KV_HEADS, HEAD_DIM)
    blocks = queries.shape[0] // TARGET_ROWS_EACH

    def step(carry, index):
        dk_total, dv_total = carry
        start = index * TARGET_ROWS_EACH

        def rows(array):
            return lax.dynamic_slice_in_dim(array, start, TARGET_ROWS_EACH, 0)
        query_tensor4 = rows(queries).astype(single_precision).reshape(TARGET_ROWS_EACH, KV_HEADS, repeat, HEAD_DIM)
        output_gradient4 = rows(cotangent).astype(single_precision).reshape(TARGET_ROWS_EACH, KV_HEADS, repeat, HEAD_DIM)
        out4 = rows(attn_out).astype(single_precision).reshape(TARGET_ROWS_EACH, KV_HEADS, repeat, HEAD_DIM)
        lse = jnp.transpose(rows(log_norm).reshape(TARGET_ROWS_EACH, KV_HEADS, repeat), (1, 2, 0))[..., None]
        delta = jnp.transpose(lax.optimization_barrier(jnp.sum(output_gradient4 * out4, axis=3)), (1, 2, 0))[..., None]
        logit_scores = jnp.einsum('znjk,wnk->njzw', query_tensor4, shared_key_heads) * score_scale
        probs = jnp.exp(logit_scores - lse)
        probabilities16 = lax.optimization_barrier(probs.astype(jnp.bfloat16)).astype(single_precision)
        prob_gradient = jnp.einsum('znjk,wnk->njzw', output_gradient4, shared_value_heads)
        score_gradient = lax.optimization_barrier((probs * (prob_gradient - delta)).astype(jnp.bfloat16)).astype(single_precision)
        query_gradient = (jnp.einsum('wohn,nwb->hwob', score_gradient, shared_key_heads) * score_scale).reshape(TARGET_ROWS_EACH, -1)
        key_gradient = jnp.einsum('nkjv,jnka->vna', score_gradient, query_tensor4) * score_scale
        value_gradient = jnp.einsum('nkjv,jnka->vna', probabilities16, output_gradient4)
        dk16 = lax.optimization_barrier(key_gradient.reshape(src_rows, -1).astype(jnp.bfloat16)).astype(single_precision)
        dv16 = lax.optimization_barrier(value_gradient.reshape(src_rows, -1).astype(jnp.bfloat16)).astype(single_precision)
        return ((dk_total + dk16, dv_total + dv16), query_gradient.astype(jnp.bfloat16))
    start_carry = (jnp.zeros((src_rows, KW), single_precision), jnp.zeros((src_rows, KW), single_precision))
    (dk_total, dv_total), dq_blocks = lax.scan(step, start_carry, jnp.arange(blocks, dtype=jnp.int32))
    dq16 = dq_blocks.reshape(queries.shape[0], -1)
    d_target = jnp.dot(dq16, w_query.T, preferred_element_type=single_precision).astype(jnp.bfloat16)
    stacked = jnp.concatenate([dk_total.astype(jnp.bfloat16), dv_total.astype(jnp.bfloat16)], axis=1)
    weights = jnp.concatenate([w_key, w_value], axis=1)
    d_source = jnp.dot(stacked, weights.T, preferred_element_type=single_precision).astype(jnp.bfloat16)
    d_wvalue = jnp.dot(source.T, dv_total.astype(jnp.bfloat16), preferred_element_type=single_precision)
    return (d_target, d_source, d_wvalue)
```

```python
import functools
import math

import jax
import jax.numpy as jnp
from jax import lax
from jax.experimental import pallas as pl
from jax.experimental.pallas import tpu as pltpu
from jax.sharding import PartitionSpec as P

HEADS = 12
KV_HEADS = 2
HEAD_DIM = 256
GROUP = HEADS // KV_HEADS
SCALE = 1.0 / math.sqrt(HEAD_DIM)
F32 = jnp.float32
BF16 = jnp.bfloat16
VMEM = pl.BlockSpec(memory_space=pltpu.VMEM)
SMEM = pl.BlockSpec(memory_space=pltpu.SMEM)


def dot(a, b, contract):
    return lax.dot_general(a, b, (contract, ((), ())), preferred_element_type=F32)


NN = ((1,), (0,))
NT = ((1,), (1,))
TN = ((0,), (0,))


def call(kernel, outs, scratch, flops, operands, specs=None, name=None):
    moved = sum(x.size * x.dtype.itemsize for x in operands)
    moved += sum(math.prod(o.shape) * o.dtype.itemsize for o in outs)
    return pl.pallas_call(
        kernel,
        out_shape=outs,
        in_specs=specs or [VMEM] * len(operands),
        out_specs=[VMEM] * len(outs),
        scratch_shapes=scratch,
        cost_estimate=pl.CostEstimate(flops=flops, bytes_accessed=moved, transcendentals=0),
        compiler_params=pltpu.CompilerParams(vmem_limit_bytes=24 * 1024 * 1024),
        name=name,
    )(*operands)


def prepare_kernel(q_ref, do_ref, o_ref, qs_ref, dos_ref, delta_ref):
    rows = q_ref.shape[0]
    lanes = lax.broadcasted_iota(jnp.int32, (rows, 128), 1)
    columns = jnp.zeros((rows, 128), F32)
    for h in range(HEADS):
        span = slice(h * HEAD_DIM, (h + 1) * HEAD_DIM)
        there = slice(h * rows, (h + 1) * rows)
        qs_ref[there, :] = q_ref[:, span]
        grad = do_ref[:, span]
        dos_ref[there, :] = grad
        total = jnp.sum(grad.astype(F32) * o_ref[:, span].astype(F32), axis=1, keepdims=True)
        columns = jnp.where(lanes == h, total, columns)
    delta_ref[...] = columns.T[: delta_ref.shape[0], :]


def chunk_kernel(tiles, blocks, each, first, last, *refs):
    n_pieces = sum(len(t) for t in tiles)
    refs = list(refs)
    start_ref, half_ref, lse_ref, delta_ref, q_ref, do_ref, wk_ref, wv_ref = refs[:8]
    source = {(0, 0): refs[8], (1, 0): refs[9], (0, 1): refs[10], (1, 1): refs[11]}
    pieces = refs[12 : 12 + n_pieces]
    refs = refs[12 + n_pieces :]
    if not first:
        old_ref = refs.pop(0)
    ds_ref, near_ref, far_ref = refs[:3]
    refs = refs[3:]
    if last:
        wv_near_ref, wv_far_ref = refs[:2]
        refs = refs[2:]
    else:
        total_ref = refs.pop(0)
    if last:
        total_ref = refs.pop()
    p_ref, dkv_ref, src_ref = refs
    width = wk_ref.shape[1]
    rows = q_ref.shape[0] // HEADS
    stacked = GROUP * rows
    step = 2 * rows
    row, index = 0, 0
    near_row, far_row = 0, 0
    fresh = first
    for tile in tiles:
        held = [pieces[i] for i in tile]
        height = sum(x.shape[0] for x in held)
        for g in range(KV_HEADS):
            cols = slice(g * HEAD_DIM, (g + 1) * HEAD_DIM)
            vcols = slice(width + g * HEAD_DIM, width + (g + 1) * HEAD_DIM)
            k = jnp.concatenate([x[:, cols] for x in held], axis=0)
            v = jnp.concatenate([x[:, vcols] for x in held], axis=0)
            for n in range(stacked // step):
                at = slice(g * stacked + n * step, g * stacked + (n + 1) * step)
                h = g * GROUP + 2 * n
                lse = jnp.concatenate([lse_ref[h : h + 1, :], lse_ref[h + 1 : h + 2, :]], axis=1)
                delta = jnp.concatenate([delta_ref[h : h + 1, :], delta_ref[h + 1 : h + 2, :]], axis=1)
                probs = jnp.exp(dot(k, q_ref[at, :], NT) * SCALE - lse)
                p_ref[:height, n * step : (n + 1) * step] = probs.astype(BF16)
                dprob = dot(v, do_ref[at, :], NT)
                ds_ref[row : row + height, at] = (probs * (dprob - delta)).astype(BF16)
            mine = slice(g * stacked, (g + 1) * stacked)
            dk = dot(ds_ref[row : row + height, mine], q_ref[mine, :], NN) * SCALE
            dkv_ref[:height, cols] = dk.astype(BF16)
            dv = dot(p_ref[:height, :], do_ref[mine, :], NN)
            dkv_ref[:height, vcols] = dv.astype(BF16)
        part = dot(dkv_ref[:height, :width], wk_ref[...], NT) + dot(dkv_ref[:height, width:], wv_ref[...], NT)
        at = 0
        for i, x in zip(tile, held):
            size = x.shape[0]
            value = part[at : at + size, :]
            if blocks[i][0][1] == 0:
                near_ref[near_row : near_row + size, :] = value
                near_row += size
            else:
                far_ref[far_row : far_row + size, :] = value.astype(BF16)
                far_row += size
            for b, owner in enumerate(blocks[i]):
                begin = pl.multiple_of(start_ref[index], each)
                src_ref[at + b * each : at + (b + 1) * each, :] = source[owner][pl.ds(begin, each), :]
                index += 1
            at += size
        term = dot(src_ref[:height, :], dkv_ref[:height, width:], TN)
        if fresh:
            total_ref[...] = term
            fresh = False
        elif row == 0:
            total_ref[...] = old_ref[...] + term
        else:
            total_ref[...] += term
        row += height
    if last:
        half = wv_near_ref.shape[0]
        mine = pl.multiple_of(half_ref[0] * half, half)
        other = pl.multiple_of((1 - half_ref[0]) * half, half)
        wv_near_ref[...] = total_ref[pl.ds(mine, half), :]
        wv_far_ref[...] = total_ref[pl.ds(other, half), :].astype(BF16)


def target_kernel(n_chunks, pieces_of, *refs):
    refs = list(refs)
    wq_ref = refs.pop(0)
    ds_refs = refs[:n_chunks]
    n_pieces = sum(pieces_of)
    pieces = refs[n_chunks : n_chunks + n_pieces]
    out_ref, kt_ref = refs[n_chunks + n_pieces :]
    rows = out_ref.shape[0]
    width = kt_ref.shape[0]
    row = 0
    for x in pieces:
        size = x.shape[0]
        kt_ref[:, row : row + size] = x[:, :width].T
        row += size
    total = jnp.zeros((out_ref.shape[1], rows), F32)
    for g in range(KV_HEADS):
        for n in range(GROUP // 2):
            h = g * GROUP + 2 * n
            dq = jnp.zeros((HEAD_DIM, 2 * rows), F32)
            row = 0
            for ds_ref in ds_refs:
                size = ds_ref.shape[0]
                keys = kt_ref[g * HEAD_DIM : (g + 1) * HEAD_DIM, row : row + size]
                dq += dot(keys, ds_ref[:, h * rows : (h + 2) * rows], NN)
                row += size
            dq = (dq * SCALE).astype(BF16)
            for i in range(2):
                cols = slice((h + i) * HEAD_DIM, (h + i + 1) * HEAD_DIM)
                total += dot(wq_ref[:, cols], dq[:, i * rows : (i + 1) * rows], NN)
    out_ref[...] = total.T.astype(BF16)


def place_kernel(n, each, *refs):
    start_ref = refs[0]
    mine, theirs, out_ref = refs[1 : 1 + n], refs[1 + n : 1 + 2 * n], refs[1 + 2 * n]
    index = 0
    for a, b in zip(mine, theirs):
        for at in range(0, a.shape[0], each):
            value = a[at : at + each, :] + b[at : at + each, :].astype(F32)
            out_ref[pl.ds(pl.multiple_of(start_ref[index], each), each), :] = value.astype(BF16)
            index += 1


def gathered(n_sp, n_tp, queries, attn_out, log_norm, cotangent, keys, values, source, w_query, w_key, w_value):
    rows = queries.shape[0]
    each, width = keys.shape
    cols = w_key.shape[0]
    shape = jax.ShapeDtypeStruct
    sp, tp = lax.axis_index("sp"), lax.axis_index("tp")
    core_ring = [(i, i ^ 1) for i in range(n_sp)]
    y_ring = [(i, i ^ 2) for i in range(n_sp)]
    x_ring = [(i, i ^ 1) for i in range(n_tp)]
    up_ring = [(i, (i + 2) % n_tp) for i in range(n_tp)]
    down_ring = [(i, (i - 2) % n_tp) for i in range(n_tp)]

    def core(a):
        return lax.ppermute(a, "sp", core_ring)

    def y(a):
        return lax.ppermute(a, "sp", y_ring)

    def x(a):
        return lax.ppermute(a, "tp", x_ring)

    def up(a):
        return lax.ppermute(a, "tp", up_ring)

    def down(a):
        return lax.ppermute(a, "tp", down_ring)

    own = jnp.concatenate([keys, values], axis=1)
    pair = jnp.concatenate([own, y(own)], axis=0)
    crossed = x(pair)
    below0, above0 = up(pair), down(pair)
    below1, above1 = up(crossed), down(crossed)
    far0, far1 = up(below0), down(above1)

    src_y = y(source)
    src = (source, src_y, core(source), core(src_y))

    qs, dos, delta = call(
        prepare_kernel,
        [shape((HEADS * rows, HEAD_DIM), BF16)] * 2 + [shape((16, rows), F32)],
        [],
        10 * queries.size,
        (queries, cotangent, attn_out),
        name="prepare",
    )
    lse = log_norm.T

    z, lane = tp // 2, tp % 2

    def place(offsets):
        dz, dx = (jnp.asarray(a, jnp.int32) for a in zip(*offsets))
        return (((z + dz) % (n_tp // 2)) * 2 + (lane ^ dx)) * each

    chunks = [
        ([pair, crossed], [(0, 0), (0, 1)]),
        ([below0, below1, above0, above1], [(-1, 0), (-1, 1), (1, 0), (1, 1)]),
        ([far0, far1], [(2, 0), (2, 1)]),
    ]
    half = jnp.reshape(sp % 2, (1,)).astype(jnp.int32)
    total = None
    all_ds, all_pieces, mine, theirs, order = [], [], [], [], []
    for c, (pieces, places) in enumerate(chunks):
        first, last = c == 0, c == len(chunks) - 1
        held, blocks, starts, tiles = [], [], [], []
        for i in range(0, len(pieces), 2):
            tiles.append([len(held) + k for k in range(4)])
            for dc in range(2):
                for k in range(2):
                    held.append(core(pieces[i + k]) if dc else pieces[i + k])
                    blocks.append([(0, dc), (1, dc)])
                    starts += [places[i + k]] * 2
        size = sum(p.shape[0] for p in held)
        height = sum(held[i].shape[0] for i in tiles[0])
        operands = [place(starts), half, lse, delta, qs, dos, w_key, w_value, *src, *held]
        outs = [shape((size, HEADS * rows), BF16), shape((size // 2, cols), F32), shape((size // 2, cols), BF16)]
        scratch = [
            pltpu.VMEM((height, GROUP * rows), BF16),
            pltpu.VMEM((height, 2 * width), BF16),
            pltpu.VMEM((height, cols), BF16),
        ]
        if not first:
            operands.append(total)
        if last:
            outs += [shape((cols // 2, width), F32), shape((cols // 2, width), BF16)]
            scratch.append(pltpu.VMEM((cols, width), F32))
        else:
            outs.append(shape((cols, width), F32))
        flops = 2 * size * rows * HEADS * HEAD_DIM * 4 + 2 * size * cols * width * 3
        results = call(
            functools.partial(chunk_kernel, tiles, blocks, each, first, last),
            outs,
            scratch,
            flops,
            operands,
            specs=[SMEM, SMEM] + [VMEM] * (len(operands) - 2),
            name=f"chunk{c}",
        )
        ds, near, far = results[:3]
        if last:
            wv_near, wv_far = results[3:]
        else:
            total = results[3]
        all_ds.append(ds)
        all_pieces.append(held)
        summed = (near + core(far).astype(F32)).reshape(-1, 2, each, cols)
        mine.append(summed[:, 0].reshape(-1, cols))
        theirs.append(y(summed[:, 1].reshape(-1, cols).astype(BF16)))
        order += places

    wv = (wv_near + core(wv_far).astype(F32)).astype(BF16)
    wv = (wv.astype(F32) + y(wv).astype(F32)).astype(BF16)
    wv_other = core(wv)
    even = sp % 2 == 0
    d_wvalue = jnp.concatenate([jnp.where(even, wv, wv_other), jnp.where(even, wv_other, wv)], axis=0).astype(F32)

    flat = [p for held in all_pieces for p in held]
    (d_target,) = call(
        functools.partial(target_kernel, len(chunks), [len(held) for held in all_pieces]),
        [shape((rows, cols), BF16)],
        [pltpu.VMEM((width, sum(p.shape[0] for p in flat)), BF16)],
        2 * rows * HEADS * HEAD_DIM * (sum(p.shape[0] for p in flat) + cols),
        (w_query, *all_ds, *flat),
        name="target",
    )
    (d_source,) = call(
        functools.partial(place_kernel, len(chunks), each),
        [shape((source.shape[0], cols), BF16)],
        [],
        2 * source.size,
        (place(order), *mine, *theirs),
        specs=[SMEM] + [VMEM] * (2 * len(chunks)),
        name="place",
    )
    return d_target, d_source, d_wvalue


def sharded(queries, attn_out, log_norm, cotangent, keys, values, source, w_query, w_key, w_value):
    rows = queries.shape[0]
    near_keys, near_values = (
        lax.all_gather(keys, "sp", axis=0, tiled=True),
        lax.all_gather(values, "sp", axis=0, tiled=True),
    )
    span = near_keys.shape[0]
    q4 = queries.reshape(rows, KV_HEADS, GROUP, HEAD_DIM)
    g4 = cotangent.reshape(rows, KV_HEADS, GROUP, HEAD_DIM)
    o4 = attn_out.reshape(rows, KV_HEADS, GROUP, HEAD_DIM)
    k3 = near_keys.reshape(span, KV_HEADS, HEAD_DIM)
    v3 = near_values.reshape(span, KV_HEADS, HEAD_DIM)
    delta = jnp.sum(g4.astype(F32) * o4.astype(F32), axis=3)
    delta = jnp.transpose(delta, (1, 2, 0))[..., None]
    lse = jnp.transpose(log_norm.reshape(rows, KV_HEADS, GROUP), (1, 2, 0))[..., None]
    scores = jnp.einsum("znjk,wnk->njzw", q4, k3, preferred_element_type=F32) * SCALE
    probs = jnp.exp(scores - lse)
    probs16 = probs.astype(BF16)
    dprob = jnp.einsum("znjk,wnk->njzw", g4, v3, preferred_element_type=F32)
    dscore = (probs * (dprob - delta)).astype(BF16)
    dq = jnp.einsum("wohn,nwb->hwob", dscore, k3, preferred_element_type=F32) * SCALE
    dk = jnp.einsum("nkjv,jnka->vna", dscore, q4, preferred_element_type=F32) * SCALE
    dv = jnp.einsum("nkjv,jnka->vna", probs16, g4, preferred_element_type=F32)
    own = [
        lax.psum_scatter(a.reshape(span, -1).astype(BF16), "sp", scatter_dimension=0, tiled=True)
        for a in (dk, dv)
    ]
    group = lax.all_gather(jnp.concatenate(own, axis=1), "tp", axis=0, tiled=True)
    weights = jnp.concatenate([w_key, w_value], axis=1)
    d_source = dot(group, weights, NT).astype(BF16)
    term = dot(source, group[:, w_value.shape[1] :], TN)
    d_wvalue = lax.psum(term.astype(BF16), "sp").astype(F32)
    dq16 = lax.psum(dq.reshape(rows, -1), "tp").astype(BF16)
    d_target = dot(dq16, w_query, NT).astype(BF16)
    return d_target, d_source, d_wvalue


def solution(mesh):
    n_sp, n_tp = mesh.shape["sp"], mesh.shape["tp"]

    def shards(*args):
        keys = args[4]
        if (n_sp, n_tp) == (4, 8) and args[0].shape[0] == 128:
            return gathered(n_sp, n_tp, *args)
        return sharded(*args)

    in_specs = (
        P("sp", None),
        P("sp", None),
        P("sp", None),
        P("sp", None),
        P(("sp", "tp"), None),
        P(("sp", "tp"), None),
        P("sp", "tp"),
        P("tp", None),
        P("tp", None),
        P("tp", None),
    )
    out_specs = (P("sp", "tp"), P("sp", "tp"), P("tp", None))
    return jax.shard_map(shards, mesh=mesh, in_specs=in_specs, out_specs=out_specs, check_vma=False)
```

```python
import functools
import math

import jax
import jax.numpy as jnp
from jax import lax
from jax.experimental import pallas as pl
from jax.experimental.pallas import tpu as pltpu
from jax.sharding import PartitionSpec as P


HEADS = 12
KV_HEADS = 2
HEAD_DIM = 256
GROUP = HEADS // KV_HEADS
SCALE = 1.0 / math.sqrt(HEAD_DIM)
F32 = jnp.float32
BF16 = jnp.bfloat16
VMEM = pl.BlockSpec(memory_space=pltpu.VMEM)
HBM = pl.BlockSpec(memory_space=pltpu.HBM)


def dot(a, b, contract):
    return lax.dot_general(a, b, (contract, ((), ())), preferred_element_type=F32)


NN = ((1,), (0,))
NT = ((1,), (1,))
TN = ((0,), (0,))


def call(kernel, outs, scratch, flops, operands, specs=None, out_specs=None):
    moved = sum(x.size * x.dtype.itemsize for x in operands)
    moved += sum(math.prod(o.shape) * o.dtype.itemsize for o in outs)
    return pl.pallas_call(
        kernel,
        out_shape=outs,
        in_specs=specs or [VMEM] * len(operands),
        out_specs=out_specs or [VMEM] * len(outs),
        scratch_shapes=scratch,
        cost_estimate=pl.CostEstimate(flops=flops, bytes_accessed=moved, transcendentals=0),
        compiler_params=pltpu.CompilerParams(vmem_limit_bytes=24 * 1024 * 1024),
    )(*operands)


def stack_kernel(*refs):
    each = refs[0].shape[0]
    for i, ref in enumerate(refs[:-1]):
        refs[-1][i * each : (i + 1) * each, :] = ref[...]


def prepare_kernel(q_ref, do_ref, o_ref, lse_ref, qs_ref, dos_ref, rows_ref):
    rows = q_ref.shape[0]
    lanes = lax.broadcasted_iota(jnp.int32, (rows, 128), 1)
    columns = jnp.zeros((rows, 128), F32)
    for h in range(HEADS):
        span = slice(h * HEAD_DIM, (h + 1) * HEAD_DIM)
        there = slice(h * rows, (h + 1) * rows)
        qs_ref[there, :] = q_ref[:, span]
        grad = do_ref[:, span]
        dos_ref[there, :] = grad
        total = jnp.sum(grad.astype(F32) * o_ref[:, span].astype(F32), axis=1, keepdims=True)
        columns = jnp.where(lanes == h, total, columns)
    rows_ref[:16, :] = columns.T[:16, :]
    rows_ref[16 : 16 + HEADS, :] = lse_ref[...]
    rows_ref[16 + HEADS :, :] = jnp.zeros((rows_ref.shape[0] - 16 - HEADS, rows), F32)


def place(dz, dx, each):
    other = jnp.bitwise_xor(lax.axis_index("tp"), jnp.int32(2 * dz) + dx)
    return pl.multiple_of(other * each, each)


def my_core():
    return lax.rem(lax.axis_index("sp"), 2)


def across(column):
    if column == "own":
        return 0, 0
    if column == "both":
        return 1, 1
    over_y = my_core() if column == 0 else 1 - my_core()
    return 1 - over_y, over_y


def pick_source(here_ref, there_ref, column, planes, each, src_ref):
    dx, dy = across(column)
    for b, dz in enumerate(planes):
        begin = pl.ds(place(dz, dx, each), each)
        if column == "own":
            value = here_ref[begin, :]
        elif column == "both":
            value = there_ref[begin, :]
        else:
            value = jnp.where(dy == 0, here_ref[begin, :], there_ref[begin, :])
        src_ref[b * each : (b + 1) * each, :] = value


def head_rows(ref, h):
    return jnp.concatenate([ref[pl.ds(h, 1), :], ref[pl.ds(h + 1, 1), :]], axis=1)


def chunk_kernel(columns, planes, each, mode, *refs):
    refs = list(refs)

    def take(n):
        out = refs[:n]
        del refs[:n]
        return out

    blocks = [take(3), take(3)]
    wk_ref, wv_ref, piece = take(3)
    source = take(2) if mode == "merge" else None
    old = take(3) if mode == "merge" else None
    given = take(2) if mode == "rest" else None
    ds_ref = take(1)[0]
    outs = take({"keep": 2, "merge": 3, "rest": 1}[mode])
    p_ref, dkv_ref, src_ref = refs
    width = wk_ref.shape[1]
    rows = blocks[0][0].shape[0] // HEADS
    stacked = GROUP * rows
    step = 2 * rows
    if given is not None:
        for x, g in zip(given, (1 - my_core(), my_core())):
            dkv_ref[:, pl.ds(pl.multiple_of(width + g * HEAD_DIM, HEAD_DIM), HEAD_DIM)] = x[...]
    for g in range(KV_HEADS):
        cols = slice(g * HEAD_DIM, (g + 1) * HEAD_DIM)
        vcols = slice(width + g * HEAD_DIM, width + (g + 1) * HEAD_DIM)
        mine = slice(g * stacked, (g + 1) * stacked)
        k, v = piece[:, cols], piece[:, vcols]
        dk = dv = 0.0
        for t, (q_ref, do_ref, rows_ref) in enumerate(blocks):
            base = t * HEADS * rows
            for n in range(stacked // step):
                at = slice(g * stacked + n * step, g * stacked + (n + 1) * step)
                h = g * GROUP + 2 * n
                probs = jnp.exp(dot(k, q_ref[at, :], NT) * SCALE - head_rows(rows_ref, 16 + h))
                if given is None:
                    p_ref[:, t * stacked + n * step : t * stacked + (n + 1) * step] = probs.astype(BF16)
                dprob = dot(v, do_ref[at, :], NT)
                grads = probs * (dprob - head_rows(rows_ref, h))
                ds_ref[:, base + at.start : base + at.stop] = grads.astype(BF16)
            dk += dot(ds_ref[:, base + mine.start : base + mine.stop], q_ref[mine, :], NN)
            if given is None:
                dv += dot(p_ref[:, t * stacked : (t + 1) * stacked], do_ref[mine, :], NN)
        dkv_ref[:, cols] = (dk * SCALE).astype(BF16)
        if given is None:
            dkv_ref[:, vcols] = dv.astype(BF16)
    part = dot(dkv_ref[:, :width], wk_ref[...], NT) + dot(dkv_ref[:, width:], wv_ref[...], NT)
    if mode == "rest":
        outs[0][...] = part.astype(BF16)
        return
    if mode == "keep":
        outs[0][...] = part
        outs[1][...] = dkv_ref[:, width:]
        return
    other_part, *gradients = old
    x_ref, y_ref, total_ref = outs
    dx, _ = across(columns[2])
    x_ref[...] = jnp.where(dx == 1, part, other_part[...])
    y_ref[...] = jnp.where(dx == 1, other_part[...], part).astype(BF16)
    total = None
    for column, dv_ref in zip(columns, (*gradients, dkv_ref.at[:, width:])):
        pick_source(*source, column, planes, each, src_ref)
        term = dot(src_ref[...], dv_ref[...], TN)
        total = term if total is None else total + term
    total_ref[...] = total


def value_kernel(column, planes, each, mine, *refs):
    blocks, refs = [refs[:3], refs[3:6]], refs[6:]
    piece, here_ref, there_ref, old_ref, dv_ref, out_ref, p_ref, src_ref = refs
    rows = blocks[0][0].shape[0] // HEADS
    stacked = GROUP * rows
    step = 2 * rows
    g = my_core() if mine else 1 - my_core()
    pick_source(here_ref, there_ref, column, planes, each, src_ref)
    cols = pl.ds(pl.multiple_of(g * HEAD_DIM, HEAD_DIM), HEAD_DIM)
    all_rows = pl.ds(pl.multiple_of(g * stacked, stacked), stacked)
    k = piece[:, cols]
    dv = 0.0
    for t, (q_ref, do_ref, rows_ref) in enumerate(blocks):
        for n in range(stacked // step):
            at = pl.ds(pl.multiple_of(g * stacked + n * step, step), step)
            lse = head_rows(rows_ref, 16 + g * GROUP + 2 * n)
            probs = jnp.exp(dot(k, q_ref[at, :], NT) * SCALE - lse)
            p_ref[:, t * stacked + n * step : t * stacked + (n + 1) * step] = probs.astype(BF16)
        dv += dot(p_ref[:, t * stacked : (t + 1) * stacked], do_ref[all_rows, :], NN)
    dv_ref[...] = dv.astype(BF16)
    out_ref[...] = (old_ref[:, cols] + dot(src_ref[...], dv_ref[...], TN)).astype(out_ref.dtype)


def target_kernel(g, n, last, *refs):
    refs = list(refs)
    wq_hbm = refs.pop(0)
    old_ref = refs.pop(0) if last else None
    ds_refs, pieces = refs[:n], refs[n : 2 * n]
    outs = refs[2 * n : -4]
    kt_ref, dq_ref, wq_ref, sem = refs[-4:]
    span = GROUP * HEAD_DIM
    copy = pltpu.make_async_copy(wq_hbm.at[:, g * span : (g + 1) * span], wq_ref, sem)
    copy.start()
    rows = ds_refs[0].shape[1] // (2 * HEADS)
    keys = jnp.concatenate([x[:, g * HEAD_DIM : (g + 1) * HEAD_DIM] for x in pieces], axis=0)
    kt_ref[...] = keys.T
    for i in range(GROUP):
        at = [(t * HEADS + g * GROUP + i) * rows for t in range(2)]
        grads = [jnp.concatenate([ds[:, x : x + rows] for x in at], axis=1) for ds in ds_refs]
        dq = dot(kt_ref[...], jnp.concatenate(grads, axis=0), NN) * SCALE
        dq_ref[i * HEAD_DIM : (i + 1) * HEAD_DIM, :] = dq.astype(BF16)
    copy.wait()
    total = dot(wq_ref[...], dq_ref[...], NN)
    if not last:
        outs[0][...] = total
        return
    total += old_ref[...]
    for t in range(2):
        outs[t][...] = total[:, t * rows : (t + 1) * rows].T


def finish_kernel(planes, each, mine_ref, other_ref, near0_ref, near1_ref, y0_ref, y1_ref, *refs):
    source_hbm, value_hbm, source_ref, value_ref, sem = refs
    half = mine_ref.shape[1]
    copies = []
    for i, (ref, which) in enumerate(((mine_ref, my_core()), (other_ref, 1 - my_core()))):
        value_ref[i] = ref[...].astype(F32)
        columns = pl.ds(pl.multiple_of(which * half, half), half)
        copies.append(pltpu.make_async_copy(value_ref.at[i], value_hbm.at[:, columns], sem.at[i]))
        copies[-1].start()
    for dx, (near_ref, y_ref) in enumerate(((near0_ref, y0_ref), (near1_ref, y1_ref))):
        for b, dz in enumerate(planes):
            span = slice(b * each, (b + 1) * each)
            value = near_ref[span, :] + y_ref[span, :].astype(F32)
            source_ref[pl.ds(place(dz, dx, each), each), :] = value.astype(BF16)
    copies.append(pltpu.make_async_copy(source_ref, source_hbm, sem.at[2]))
    copies[-1].start()
    for copy in copies:
        copy.wait()


def gathered(n_sp, n_tp, queries, attn_out, log_norm, cotangent, keys, values, source, w_query, w_key, w_value):
    rows = queries.shape[0]
    each, width = keys.shape
    cols = w_key.shape[0]
    shape = jax.ShapeDtypeStruct
    everyone = range(n_sp * n_tp)

    def across(i, first):
        return i ^ 1 if i // n_tp % 2 == first else i ^ (2 * n_tp)

    rings = {
        "core": ("sp", [(i, i ^ 1) for i in range(n_sp)]),
        "y": ("sp", [(i, i ^ 2) for i in range(n_sp)]),
        "xy": (("sp", "tp"), [(i, across(i, 0)) for i in everyone]),
        "yx": (("sp", "tp"), [(i, across(i, 1)) for i in everyone]),
    }
    planes = range(n_tp // 2)
    for dz in planes[1:]:
        rings[f"z{dz}"] = ("tp", [(i, i ^ (2 * dz)) for i in range(n_tp)])

    def move(ring, a):
        axis, pairs = rings[ring]
        return lax.ppermute(a, axis, pairs)

    own = jnp.maximum(
        lax.pad(keys, jnp.asarray(-jnp.inf, keys.dtype), ((0, 0, 0), (0, width, 0))),
        lax.pad(values, jnp.asarray(-jnp.inf, values.dtype), ((0, 0, 0), (width, 0, 0))),
    )
    (held,) = call(stack_kernel, [shape(own.shape, BF16)], [], 5 * 10**9, (own,))
    qs, dos, head = call(
        prepare_kernel,
        [shape((HEADS * rows, HEAD_DIM), BF16)] * 2 + [shape((32, rows), F32)],
        [],
        10 * queries.size,
        (queries, cotangent, attn_out, log_norm.T),
    )
    targets = [qs, dos, head]
    targets += [move("core", a) for a in (qs, dos, head)]

    (column,) = call(
        stack_kernel,
        [shape((len(planes) * each, 2 * width), BF16)],
        [],
        10**6,
        [held] + [move(f"z{dz}", own) for dz in planes[1:]],
    )
    near_a = move("xy", column)
    near_b = move("yx", column)
    diagonal = move("yx", near_a)
    pieces = (column, near_a, near_b, diagonal)
    columns = ("own", 0, 1, "both")
    src = (source, move("y", source))

    size = column.shape[0]
    flops = 4 * size * rows * HEADS * HEAD_DIM * 4 + 2 * size * cols * width * 3
    part_f32, part_bf16 = shape((size, cols), F32), shape((size, cols), BF16)

    def chunk(c, mode, outs, extra):
        return call(
            functools.partial(chunk_kernel, columns[: c + 1], planes, each, mode),
            [shape((size, 2 * HEADS * rows), BF16)] + outs,
            [
                pltpu.VMEM((size, 2 * GROUP * rows), BF16),
                pltpu.VMEM((size, 2 * width), BF16),
                pltpu.VMEM((size, cols), BF16),
            ],
            flops,
            [*targets, w_key, w_value, pieces[c], *extra],
        )

    grads = shape((size, width), BF16)
    ds0, near0, dv0 = chunk(0, "keep", [part_f32, grads], ())
    ds1, part1, dv1 = chunk(1, "keep", [part_f32, grads], ())
    ds2, near1, far0, total = chunk(
        2, "merge", [part_f32, part_bf16, shape((cols, width), F32)], (*src, part1, dv0, dv1)
    )
    y0 = move("y", far0)
    given, sides = [], []
    for i, kind in enumerate((BF16, F32)):
        dv, side = call(
            functools.partial(value_kernel, columns[3], planes, each, i == 1),
            [shape((size, HEAD_DIM), BF16), shape((cols, HEAD_DIM), kind)],
            [pltpu.VMEM((size, 2 * GROUP * rows), BF16), pltpu.VMEM((size, cols), BF16)],
            flops // 5,
            [*targets, diagonal, *src, total],
        )
        given.append(dv)
        sides.append(side)
    ds3, far1 = chunk(3, "rest", [part_bf16], given)
    y1 = move("y", far1)

    wv = (sides[1] + move("core", sides[0]).astype(F32)).astype(BF16)
    wv = (wv.astype(F32) + move("y", wv).astype(F32)).astype(BF16)
    wv_other = move("core", wv)

    all_ds = (ds0, ds1, ds2, ds3)
    terms = None
    for g in range(KV_HEADS):
        last = g == KV_HEADS - 1
        terms = call(
            functools.partial(target_kernel, g, len(all_ds), last),
            [shape((rows, cols), F32)] * 2 if last else [shape((cols, 2 * rows), F32)],
            [
                pltpu.VMEM((HEAD_DIM, size * len(pieces)), BF16),
                pltpu.VMEM((GROUP * HEAD_DIM, 2 * rows), BF16),
                pltpu.VMEM((cols, GROUP * HEAD_DIM), BF16),
                pltpu.SemaphoreType.DMA,
            ],
            4 * rows * GROUP * HEAD_DIM * (size * len(pieces) + cols),
            (w_query, *(terms if last else ()), *all_ds, *pieces),
            specs=[HBM] + [VMEM] * (2 * len(pieces) + last),
        )
    d_target = (terms[0] + move("core", terms[1])).astype(BF16)
    d_source, d_wvalue = call(
        functools.partial(finish_kernel, planes, each),
        [shape((source.shape[0], cols), BF16), shape((cols, width), F32)],
        [
            pltpu.VMEM((source.shape[0], cols), BF16),
            pltpu.VMEM((2, cols, HEAD_DIM), F32),
            pltpu.SemaphoreType.DMA((3,)),
        ],
        2 * source.size,
        (wv, wv_other, near0, near1, y0, y1),
        out_specs=[HBM] * 2,
    )
    return d_target, d_source, d_wvalue


def sharded(queries, attn_out, log_norm, cotangent, keys, values, source, w_query, w_key, w_value):
    rows = queries.shape[0]
    near_keys, near_values = (
        lax.all_gather(keys, "sp", axis=0, tiled=True),
        lax.all_gather(values, "sp", axis=0, tiled=True),
    )
    span = near_keys.shape[0]
    q4 = queries.reshape(rows, KV_HEADS, GROUP, HEAD_DIM)
    g4 = cotangent.reshape(rows, KV_HEADS, GROUP, HEAD_DIM)
    o4 = attn_out.reshape(rows, KV_HEADS, GROUP, HEAD_DIM)
    k3 = near_keys.reshape(span, KV_HEADS, HEAD_DIM)
    v3 = near_values.reshape(span, KV_HEADS, HEAD_DIM)
    delta = jnp.sum(g4.astype(F32) * o4.astype(F32), axis=3)
    delta = jnp.transpose(delta, (1, 2, 0))[..., None]
    lse = jnp.transpose(log_norm.reshape(rows, KV_HEADS, GROUP), (1, 2, 0))[..., None]
    scores = jnp.einsum("znjk,wnk->njzw", q4, k3, preferred_element_type=F32) * SCALE
    probs = jnp.exp(scores - lse)
    probs16 = probs.astype(BF16)
    dprob = jnp.einsum("znjk,wnk->njzw", g4, v3, preferred_element_type=F32)
    dscore = (probs * (dprob - delta)).astype(BF16)
    dq = jnp.einsum("wohn,nwb->hwob", dscore, k3, preferred_element_type=F32) * SCALE
    dk = jnp.einsum("nkjv,jnka->vna", dscore, q4, preferred_element_type=F32) * SCALE
    dv = jnp.einsum("nkjv,jnka->vna", probs16, g4, preferred_element_type=F32)
    own = [
        lax.psum_scatter(a.reshape(span, -1).astype(BF16), "sp", scatter_dimension=0, tiled=True)
        for a in (dk, dv)
    ]
    group = lax.all_gather(jnp.concatenate(own, axis=1), "tp", axis=0, tiled=True)
    weights = jnp.concatenate([w_key, w_value], axis=1)
    d_source = dot(group, weights, NT).astype(BF16)
    term = dot(source, group[:, w_value.shape[1] :], TN)
    d_wvalue = lax.psum(term.astype(BF16), "sp").astype(F32)
    dq16 = lax.psum(dq.reshape(rows, -1), "tp").astype(BF16)
    d_target = dot(dq16, w_query, NT).astype(BF16)
    return d_target, d_source, d_wvalue


def solution(mesh):
    n_sp, n_tp = mesh.shape["sp"], mesh.shape["tp"]
    near = (n_sp, n_tp) == (4, 8)

    def shards(*args):
        if not near:
            return sharded(*args)
        return gathered(n_sp, n_tp, *args)

    in_specs = (
        P("sp", None),
        P("sp", None),
        P("sp", None),
        P("sp", None),
        P(("sp", "tp"), None),
        P(("sp", "tp"), None),
        P("sp", "tp"),
        P("tp", None),
        P("tp", None),
        P("tp", None),
    )
    out_specs = (P("sp", "tp"), P("sp", "tp"), P("tp", None))
    return jax.shard_map(shards, mesh=mesh, in_specs=in_specs, out_specs=out_specs, check_vma=False)
```

```python
import functools
import math

import jax
import jax.numpy as jnp
from jax import lax
from jax.experimental import pallas as pl
from jax.experimental.pallas import tpu as pltpu
from jax.sharding import PartitionSpec as P


HEADS = 12
KV_HEADS = 2
HEAD_DIM = 256
GROUP = HEADS // KV_HEADS
SCALE = 1.0 / math.sqrt(HEAD_DIM)
F32 = jnp.float32
BF16 = jnp.bfloat16
VMEM = pl.BlockSpec(memory_space=pltpu.VMEM)
HBM = pl.BlockSpec(memory_space=pltpu.HBM)


def dot(a, b, contract):
    return lax.dot_general(a, b, (contract, ((), ())), preferred_element_type=F32)


NN = ((1,), (0,))
NT = ((1,), (1,))
TN = ((0,), (0,))


def call(kernel, outs, scratch, flops, operands, specs=None, out_specs=None):
    moved = sum(x.size * x.dtype.itemsize for x in operands)
    moved += sum(math.prod(o.shape) * o.dtype.itemsize for o in outs)
    return pl.pallas_call(
        kernel,
        out_shape=outs,
        in_specs=specs or [VMEM] * len(operands),
        out_specs=out_specs or [VMEM] * len(outs),
        scratch_shapes=scratch,
        cost_estimate=pl.CostEstimate(flops=flops, bytes_accessed=moved, transcendentals=0),
        compiler_params=pltpu.CompilerParams(vmem_limit_bytes=24 * 1024 * 1024),
    )(*operands)


def stack_kernel(*refs):
    each = refs[0].shape[0]
    for i, ref in enumerate(refs[:-1]):
        refs[-1][i * each : (i + 1) * each, :] = ref[...]


def prepare_kernel(q_ref, do_ref, o_ref, lse_ref, qs_ref, dos_ref, rows_ref):
    rows = q_ref.shape[0]
    lanes = lax.broadcasted_iota(jnp.int32, (rows, 128), 1)
    columns = jnp.zeros((rows, 128), F32)
    for h in range(HEADS):
        span = slice(h * HEAD_DIM, (h + 1) * HEAD_DIM)
        there = slice(h * rows, (h + 1) * rows)
        qs_ref[there, :] = q_ref[:, span]
        grad = do_ref[:, span]
        dos_ref[there, :] = grad
        total = jnp.sum(grad.astype(F32) * o_ref[:, span].astype(F32), axis=1, keepdims=True)
        columns = jnp.where(lanes == h, total, columns)
    rows_ref[:16, :] = columns.T[:16, :]
    rows_ref[16 : 16 + HEADS, :] = lse_ref[...]
    rows_ref[16 + HEADS :, :] = jnp.zeros((rows_ref.shape[0] - 16 - HEADS, rows), F32)


def place(dz, dx, each):
    other = jnp.bitwise_xor(lax.axis_index("tp"), jnp.int32(2 * dz) + dx)
    return pl.multiple_of(other * each, each)


def my_core():
    return lax.rem(lax.axis_index("sp"), 2)


def across(column):
    if column == "own":
        return 0, 0
    if column == "both":
        return 1, 1
    over_y = my_core() if column == 0 else 1 - my_core()
    return 1 - over_y, over_y


def pick_source(here_ref, there_ref, column, planes, each, src_ref):
    dx, dy = across(column)
    for b, dz in enumerate(planes):
        begin = pl.ds(place(dz, dx, each), each)
        if column == "own":
            value = here_ref[begin, :]
        elif column == "both":
            value = there_ref[begin, :]
        else:
            value = jnp.where(dy == 0, here_ref[begin, :], there_ref[begin, :])
        src_ref[b * each : (b + 1) * each, :] = value


def head_rows(ref, h):
    return jnp.concatenate([ref[pl.ds(h, 1), :], ref[pl.ds(h + 1, 1), :]], axis=1)


def chunk_kernel(columns, planes, each, mode, *refs):
    refs = list(refs)

    def take(n):
        out = refs[:n]
        del refs[:n]
        return out

    blocks = [take(3), take(3)]
    wk_ref, wv_ref, piece = take(3)
    source = take({"first": 1, "merge": 2}.get(mode, 0))
    old = take(3) if mode == "merge" else None
    given = take(2) if mode == "rest" else None
    ds_ref = take(1)[0]
    outs = take({"first": 2, "keep": 2, "merge": 3, "rest": 1}[mode])
    p_ref, dkv_ref, src_ref = refs
    width = wk_ref.shape[1]
    rows = blocks[0][0].shape[0] // HEADS
    stacked = GROUP * rows
    step = 2 * rows
    size = piece.shape[0]
    if given is not None:
        for x, g in zip(given, (1 - my_core(), my_core())):
            dkv_ref[:, pl.ds(pl.multiple_of(width + g * HEAD_DIM, HEAD_DIM), HEAD_DIM)] = x[...]
    for g in range(KV_HEADS):
        cols = slice(g * HEAD_DIM, (g + 1) * HEAD_DIM)
        vcols = slice(width + g * HEAD_DIM, width + (g + 1) * HEAD_DIM)
        mine = slice(g * stacked, (g + 1) * stacked)
        k, v = piece[:, cols], piece[:, vcols]
        dk = dv = 0.0
        for t, (q_ref, do_ref, rows_ref) in enumerate(blocks):
            base = t * HEADS * rows
            for n in range(stacked // step):
                at = slice(g * stacked + n * step, g * stacked + (n + 1) * step)
                h = g * GROUP + 2 * n
                probs = jnp.exp(dot(k, q_ref[at, :], NT) * SCALE - head_rows(rows_ref, 16 + h))
                if given is None:
                    p_ref[:, t * stacked + n * step : t * stacked + (n + 1) * step] = probs.astype(BF16)
                dprob = dot(v, do_ref[at, :], NT)
                grads = probs * (dprob - head_rows(rows_ref, h))
                ds_ref[:, base + at.start : base + at.stop] = grads.astype(BF16)
            dk += dot(ds_ref[:, base + mine.start : base + mine.stop], q_ref[mine, :], NN)
            if given is None:
                dv += dot(p_ref[:, t * stacked : (t + 1) * stacked], do_ref[mine, :], NN)
        dkv_ref[:, cols] = (dk * SCALE).astype(BF16)
        if given is None:
            dkv_ref[:, vcols] = dv.astype(BF16)
    part = dot(dkv_ref[:, :width], wk_ref[...], NT) + dot(dkv_ref[:, width:], wv_ref[...], NT)
    if mode == "rest":
        outs[0][...] = part.astype(BF16)
        return
    if mode == "first":
        outs[0][...] = part
        pick_source(source[0], None, columns[0], planes, each, src_ref.at[:size, :])
        outs[1][...] = dot(src_ref[:size, :], dkv_ref[:, width:], TN)
        return
    if mode == "keep":
        outs[0][...] = part
        outs[1][...] = dkv_ref[:, width:]
        return
    other_part, old_total, other_grads = old
    x_ref, y_ref, total_ref = outs
    dx, _ = across(columns[2])
    x_ref[...] = jnp.where(dx == 1, part, other_part[...])
    y_ref[...] = jnp.where(dx == 1, other_part[...], part).astype(BF16)
    for i in range(2):
        pick_source(*source, columns[1 + i], planes, each, src_ref.at[i * size : (i + 1) * size, :])
    both = jnp.concatenate([other_grads[...], dkv_ref[:, width:]], axis=0)
    total_ref[...] = old_total[...] + dot(src_ref[...], both, TN)


def value_kernel(column, planes, each, mine, *refs):
    blocks, refs = [refs[:3], refs[3:6]], refs[6:]
    piece, here_ref, there_ref, old_ref, dv_ref, out_ref, p_ref, src_ref = refs
    rows = blocks[0][0].shape[0] // HEADS
    stacked = GROUP * rows
    step = 2 * rows
    g = my_core() if mine else 1 - my_core()
    pick_source(here_ref, there_ref, column, planes, each, src_ref)
    cols = pl.ds(pl.multiple_of(g * HEAD_DIM, HEAD_DIM), HEAD_DIM)
    all_rows = pl.ds(pl.multiple_of(g * stacked, stacked), stacked)
    k = piece[:, cols]
    dv = 0.0
    for t, (q_ref, do_ref, rows_ref) in enumerate(blocks):
        for n in range(stacked // step):
            at = pl.ds(pl.multiple_of(g * stacked + n * step, step), step)
            lse = head_rows(rows_ref, 16 + g * GROUP + 2 * n)
            probs = jnp.exp(dot(k, q_ref[at, :], NT) * SCALE - lse)
            p_ref[:, t * stacked + n * step : t * stacked + (n + 1) * step] = probs.astype(BF16)
        dv += dot(p_ref[:, t * stacked : (t + 1) * stacked], do_ref[all_rows, :], NN)
    dv_ref[...] = dv.astype(BF16)
    out_ref[...] = (old_ref[:, cols] + dot(src_ref[...], dv_ref[...], TN)).astype(out_ref.dtype)


def target_kernel(g, n, last, *refs):
    refs = list(refs)
    wq_hbm = refs.pop(0)
    old_ref = refs.pop(0) if last else None
    ds_refs, pieces = refs[:n], refs[n : 2 * n]
    outs = refs[2 * n : -4]
    kt_ref, dq_ref, wq_ref, sem = refs[-4:]
    span = GROUP * HEAD_DIM
    copy = pltpu.make_async_copy(wq_hbm.at[:, g * span : (g + 1) * span], wq_ref, sem)
    copy.start()
    rows = ds_refs[0].shape[1] // (2 * HEADS)
    keys = jnp.concatenate([x[:, g * HEAD_DIM : (g + 1) * HEAD_DIM] for x in pieces], axis=0)
    kt_ref[...] = keys.T
    for i in range(GROUP):
        at = [(t * HEADS + g * GROUP + i) * rows for t in range(2)]
        grads = [jnp.concatenate([ds[:, x : x + rows] for x in at], axis=1) for ds in ds_refs]
        dq = dot(kt_ref[...], jnp.concatenate(grads, axis=0), NN) * SCALE
        dq_ref[i * HEAD_DIM : (i + 1) * HEAD_DIM, :] = dq.astype(BF16)
    copy.wait()
    total = dot(wq_ref[...], dq_ref[...], NN)
    if not last:
        outs[0][...] = total
        return
    total += old_ref[...]
    for t in range(2):
        outs[t][...] = total[:, t * rows : (t + 1) * rows].T


def finish_kernel(planes, each, mine_ref, other_ref, near0_ref, near1_ref, y0_ref, y1_ref, *refs):
    source_hbm, value_hbm, source_ref, value_ref, sem = refs
    half = mine_ref.shape[1]
    copies = []
    for i, (ref, which) in enumerate(((mine_ref, my_core()), (other_ref, 1 - my_core()))):
        value_ref[i] = ref[...].astype(F32)
        columns = pl.ds(pl.multiple_of(which * half, half), half)
        copies.append(pltpu.make_async_copy(value_ref.at[i], value_hbm.at[:, columns], sem.at[i]))
        copies[-1].start()
    for dx, (near_ref, y_ref) in enumerate(((near0_ref, y0_ref), (near1_ref, y1_ref))):
        for b, dz in enumerate(planes):
            span = slice(b * each, (b + 1) * each)
            value = near_ref[span, :] + y_ref[span, :].astype(F32)
            source_ref[pl.ds(place(dz, dx, each), each), :] = value.astype(BF16)
    copies.append(pltpu.make_async_copy(source_ref, source_hbm, sem.at[2]))
    copies[-1].start()
    for copy in copies:
        copy.wait()


def gathered(n_sp, n_tp, queries, attn_out, log_norm, cotangent, keys, values, source, w_query, w_key, w_value):
    rows = queries.shape[0]
    each, width = keys.shape
    cols = w_key.shape[0]
    shape = jax.ShapeDtypeStruct
    everyone = range(n_sp * n_tp)

    def across(i, first):
        return i ^ 1 if i // n_tp % 2 == first else i ^ (2 * n_tp)

    rings = {
        "core": ("sp", [(i, i ^ 1) for i in range(n_sp)]),
        "y": ("sp", [(i, i ^ 2) for i in range(n_sp)]),
        "xy": (("sp", "tp"), [(i, across(i, 0)) for i in everyone]),
        "yx": (("sp", "tp"), [(i, across(i, 1)) for i in everyone]),
    }
    planes = range(n_tp // 2)
    for dz in planes[1:]:
        rings[f"z{dz}"] = ("tp", [(i, i ^ (2 * dz)) for i in range(n_tp)])

    def move(ring, a):
        axis, pairs = rings[ring]
        return lax.ppermute(a, axis, pairs)

    own = jnp.maximum(
        lax.pad(keys, jnp.asarray(-jnp.inf, keys.dtype), ((0, 0, 0), (0, width, 0))),
        lax.pad(values, jnp.asarray(-jnp.inf, values.dtype), ((0, 0, 0), (width, 0, 0))),
    )
    (held,) = call(stack_kernel, [shape(own.shape, BF16)], [], 5 * 10**9, (own,))
    qs, dos, head = call(
        prepare_kernel,
        [shape((HEADS * rows, HEAD_DIM), BF16)] * 2 + [shape((32, rows), F32)],
        [],
        10 * queries.size,
        (queries, cotangent, attn_out, log_norm.T),
    )
    targets = [qs, dos, head]
    targets += [move("core", a) for a in (qs, dos, head)]

    (column,) = call(
        stack_kernel,
        [shape((len(planes) * each, 2 * width), BF16)],
        [],
        10**6,
        [held] + [move(f"z{dz}", own) for dz in planes[1:]],
    )
    near_a = move("xy", column)
    near_b = move("yx", column)
    diagonal = move("yx", near_a)
    pieces = (column, near_a, near_b, diagonal)
    columns = ("own", 0, 1, "both")
    src = (source, move("y", source))

    size = column.shape[0]
    flops = 4 * size * rows * HEADS * HEAD_DIM * 4 + 2 * size * cols * width * 3
    part_f32, part_bf16 = shape((size, cols), F32), shape((size, cols), BF16)

    def chunk(c, mode, outs, extra):
        return call(
            functools.partial(chunk_kernel, columns[: c + 1], planes, each, mode),
            [shape((size, 2 * HEADS * rows), BF16)] + outs,
            [
                pltpu.VMEM((size, 2 * GROUP * rows), BF16),
                pltpu.VMEM((size, 2 * width), BF16),
                pltpu.VMEM((2 * size, cols), BF16),
            ],
            flops,
            [*targets, w_key, w_value, pieces[c], *extra],
        )

    grads = shape((size, width), BF16)
    wv_shape = shape((cols, width), F32)
    ds0, near0, total = chunk(0, "first", [part_f32, wv_shape], src[:1])
    ds1, part1, dv1 = chunk(1, "keep", [part_f32, grads], ())
    ds2, near1, far0, total = chunk(
        2, "merge", [part_f32, part_bf16, wv_shape], (*src, part1, total, dv1)
    )
    y0 = move("y", far0)
    given, sides = [], []
    for i, kind in enumerate((BF16, F32)):
        dv, side = call(
            functools.partial(value_kernel, columns[3], planes, each, i == 1),
            [shape((size, HEAD_DIM), BF16), shape((cols, HEAD_DIM), kind)],
            [pltpu.VMEM((size, 2 * GROUP * rows), BF16), pltpu.VMEM((size, cols), BF16)],
            flops // 5,
            [*targets, diagonal, *src, total],
        )
        given.append(dv)
        sides.append(side)
    ds3, far1 = chunk(3, "rest", [part_bf16], given)
    y1 = move("y", far1)

    wv = (sides[1] + move("core", sides[0]).astype(F32)).astype(BF16)
    wv = (wv.astype(F32) + move("y", wv).astype(F32)).astype(BF16)
    wv_other = move("core", wv)

    all_ds = (ds0, ds1, ds2, ds3)
    terms = None
    for g in range(KV_HEADS):
        last = g == KV_HEADS - 1
        terms = call(
            functools.partial(target_kernel, g, len(all_ds), last),
            [shape((rows, cols), F32)] * 2 if last else [shape((cols, 2 * rows), F32)],
            [
                pltpu.VMEM((HEAD_DIM, size * len(pieces)), BF16),
                pltpu.VMEM((GROUP * HEAD_DIM, 2 * rows), BF16),
                pltpu.VMEM((cols, GROUP * HEAD_DIM), BF16),
                pltpu.SemaphoreType.DMA,
            ],
            4 * rows * GROUP * HEAD_DIM * (size * len(pieces) + cols),
            (w_query, *(terms if last else ()), *all_ds, *pieces),
            specs=[HBM] + [VMEM] * (2 * len(pieces) + last),
        )
    d_target = (terms[0] + move("core", terms[1])).astype(BF16)
    d_source, d_wvalue = call(
        functools.partial(finish_kernel, planes, each),
        [shape((source.shape[0], cols), BF16), shape((cols, width), F32)],
        [
            pltpu.VMEM((source.shape[0], cols), BF16),
            pltpu.VMEM((2, cols, HEAD_DIM), F32),
            pltpu.SemaphoreType.DMA((3,)),
        ],
        2 * source.size,
        (wv, wv_other, near0, near1, y0, y1),
        out_specs=[HBM] * 2,
    )
    return d_target, d_source, d_wvalue


def sharded(queries, attn_out, log_norm, cotangent, keys, values, source, w_query, w_key, w_value):
    rows = queries.shape[0]
    near_keys, near_values = (
        lax.all_gather(keys, "sp", axis=0, tiled=True),
        lax.all_gather(values, "sp", axis=0, tiled=True),
    )
    span = near_keys.shape[0]
    q4 = queries.reshape(rows, KV_HEADS, GROUP, HEAD_DIM)
    g4 = cotangent.reshape(rows, KV_HEADS, GROUP, HEAD_DIM)
    o4 = attn_out.reshape(rows, KV_HEADS, GROUP, HEAD_DIM)
    k3 = near_keys.reshape(span, KV_HEADS, HEAD_DIM)
    v3 = near_values.reshape(span, KV_HEADS, HEAD_DIM)
    delta = jnp.sum(g4.astype(F32) * o4.astype(F32), axis=3)
    delta = jnp.transpose(delta, (1, 2, 0))[..., None]
    lse = jnp.transpose(log_norm.reshape(rows, KV_HEADS, GROUP), (1, 2, 0))[..., None]
    scores = jnp.einsum("znjk,wnk->njzw", q4, k3, preferred_element_type=F32) * SCALE
    probs = jnp.exp(scores - lse)
    probs16 = probs.astype(BF16)
    dprob = jnp.einsum("znjk,wnk->njzw", g4, v3, preferred_element_type=F32)
    dscore = (probs * (dprob - delta)).astype(BF16)
    dq = jnp.einsum("wohn,nwb->hwob", dscore, k3, preferred_element_type=F32) * SCALE
    dk = jnp.einsum("nkjv,jnka->vna", dscore, q4, preferred_element_type=F32) * SCALE
    dv = jnp.einsum("nkjv,jnka->vna", probs16, g4, preferred_element_type=F32)
    own = [
        lax.psum_scatter(a.reshape(span, -1).astype(BF16), "sp", scatter_dimension=0, tiled=True)
        for a in (dk, dv)
    ]
    group = lax.all_gather(jnp.concatenate(own, axis=1), "tp", axis=0, tiled=True)
    weights = jnp.concatenate([w_key, w_value], axis=1)
    d_source = dot(group, weights, NT).astype(BF16)
    term = dot(source, group[:, w_value.shape[1] :], TN)
    d_wvalue = lax.psum(term.astype(BF16), "sp").astype(F32)
    dq16 = lax.psum(dq.reshape(rows, -1), "tp").astype(BF16)
    d_target = dot(dq16, w_query, NT).astype(BF16)
    return d_target, d_source, d_wvalue


def solution(mesh):
    n_sp, n_tp = mesh.shape["sp"], mesh.shape["tp"]
    near = (n_sp, n_tp) == (4, 8)

    def shards(*args):
        if not near:
            return sharded(*args)
        return gathered(n_sp, n_tp, *args)

    in_specs = (
        P("sp", None),
        P("sp", None),
        P("sp", None),
        P("sp", None),
        P(("sp", "tp"), None),
        P(("sp", "tp"), None),
        P("sp", "tp"),
        P("tp", None),
        P("tp", None),
        P("tp", None),
    )
    out_specs = (P("sp", "tp"), P("sp", "tp"), P("tp", None))
    return jax.shard_map(shards, mesh=mesh, in_specs=in_specs, out_specs=out_specs, check_vma=False)
```
